32 devices in a mesh: sp: 8 (over z, y), tp: 4 (over x, core).
Axes of the slice: x: 2, y: 2, z: 4, core: 2. Of those that a mesh axis runs over, the one named last changes fastest.
Arguments:
- mixer_value_projection: bfloat16 [6144, 2048], P('sp', 'tp'), may hold values from -6 to 6
- write_vectors_projected: bfloat16 [6144, 256], P('sp', 'tp'), may hold values from -6 to 6
- read_vectors_projected: bfloat16 [6144, 256], P('sp', 'tp'), may hold values from -6 to 6
- output_gate_projected: bfloat16 [6144, 2048], P('sp', 'tp'), may hold values from -6 to 6
- step_size_scores: float32 [6144, 32], P('sp', 'tp'), may hold values from -8 to 8
- position_decay_extra: float32 [6144, 32], P('sp', 'tp'), may hold values from -1 to 0
- step_size_bias: float32 [32], P('tp'), may hold values from -1 to 1
- head_decay_logarithm: float32 [32], P('tp'), may hold values from -14 to -3
- value_filter_taps: bfloat16 [4, 2048], P(None, 'tp'), may hold values from -3 to 3
- write_filter_taps: bfloat16 [4, 256], P(None, 'tp'), may hold values from -3 to 3
- read_filter_taps: bfloat16 [4, 256], P(None, 'tp'), may hold values from -3 to 3
- gated_group_norm_gain: float32 [2048], P('tp'), may hold values from 0.1 to 1.9
- mixer_output_weight: bfloat16 [2048, 2048], P('tp'), may hold values from -0.125 to 0.125
- residual: bfloat16 [6144, 2048], P('sp'), may hold values from -6 to 6
- feedforward_norm_gain: float32 [2048], replicated, may hold values from 0.1 to 1.9
- feedforward_gate_weight: bfloat16 [2048, 5632], P('sp', 'tp'), may hold values from -0.125 to 0.125
- feedforward_value_weight: bfloat16 [2048, 5632], P('sp', 'tp'), may hold values from -0.125 to 0.125
- gate_filter_taps: bfloat16 [3, 5632], P(None, 'tp'), may hold values from -3.5 to 3.5
- single_value_filter_taps: bfloat16 [3, 5632], P(None, 'tp'), may hold values from -3.5 to 3.5
- feedforward_down_weight: bfloat16 [5632, 2048], P('tp', 'sp'), may hold values from -0.078125 to 0.078125
Outputs:
- mixed: bfloat16 [6144, 2048], P(('sp', 'tp'))
The draws below stay inside these ranges and needn't reach their ends.
All inputs are finite; a program needn't handle non-finite values.
Results may differ from the reference program's by a relative error of at most 0.012.
Values may be sent and summed in bfloat16 or wider, within the bound.
A program may use at most 192 MiB of HBM per device.

```python
import jax
import jax.numpy as jnp
from jax import lax

D = 2048
HEADS = 32
HEAD = 64
GROUPS = 4
STATE = 64
FF = 5632
TOK_DEV = 768
BLOCK = 128
CONV_MIX = 4
CONV_FFN = 3
INNER = 2048
SEQ = 6144


def draw_step_size_scores(key, part):
    first, second = jax.random.split(jax.random.fold_in(key, 11))
    block_total = SEQ // TOK_DEV
    base = jax.random.normal(first, (SEQ, HEADS), jnp.float32)
    shifts = jax.random.uniform(second, (block_total, 1, HEADS), jnp.float32, -1.5, 1.5)
    return (base.reshape(block_total, TOK_DEV, HEADS) + shifts).reshape(SEQ, HEADS)


def draw_head_decay_logarithm(key, part):
    first, second, third = jax.random.split(jax.random.fold_in(key, 12), 3)
    share = 0.5
    slowly = jax.random.uniform(first, (HEADS,), jnp.float32) < share
    slow_rate = jnp.log(jax.random.uniform(second, (HEADS,), jnp.float32, 0.4, 1.0) / SEQ)
    fast_rate = jax.random.uniform(third, (HEADS,), jnp.float32, jnp.log(1.0 / 60.0), jnp.log(1.0 / 25.0))
    return jnp.where(slowly, slow_rate, fast_rate)


def draw_position_decay_extra(key, part):
    first, second = jax.random.split(jax.random.fold_in(key, 13))
    places = jax.random.randint(first, (3,), 0, SEQ)
    losses = jnp.log(jax.random.uniform(second, (3, HEADS), jnp.float32, 0.5, 0.8))
    positions = jnp.arange(SEQ)
    hits = (positions[:, None] == places[None, :]).astype(jnp.float32)
    return jnp.sum(hits[:, :, None] * losses[None, :, :], axis=1)


def block_levels(rng, dims, cuts, smallest, top_value):
    level = 1.0
    for position, parts in cuts:
        heights = jax.random.uniform(jax.random.fold_in(jax.random.fold_in(rng, 6), position), (parts,), jnp.float32, smallest / len(cuts), top_value / len(cuts))
        level = level * jnp.repeat(jnp.exp(heights), dims[position] // parts).reshape((-1,) + (1,) * (len(dims) - 1 - position))
    return level


def scatter_about(own_key, extent, deviation, bound, pieces=(), held_as=jnp.bfloat16):
    loudness = block_levels(own_key, extent, pieces, -0.22, 0.18) if pieces else 1.0
    array = jax.random.normal(own_key, extent, jnp.float32) * deviation * loudness
    return jnp.minimum(jnp.maximum(array, -bound), bound).astype(held_as)


def setup_inputs(seed: int = 0) -> dict:
    streams_of = jax.random.split(jax.random.key(seed), 21)
    mixer_value_projection = scatter_about(streams_of[0], (SEQ, INNER), 1.0, 6.0, ((0, 8), (1, 4)))
    write_vectors_projected = scatter_about(streams_of[1], (SEQ, GROUPS * STATE), 1.0, 6.0, ((0, 8), (1, 4)))
    read_vectors_projected = scatter_about(streams_of[2], (SEQ, GROUPS * STATE), 1.0, 6.0, ((0, 8), (1, 4)))
    output_gate_projected = scatter_about(streams_of[3], (SEQ, INNER), 1.0, 6.0, ((0, 8), (1, 4)))
    step_size_scores = draw_step_size_scores(jax.random.fold_in(streams_of[20], 71), 0)
    position_decay_extra = draw_position_decay_extra(jax.random.fold_in(streams_of[20], 71), 0)
    step_size_bias = jnp.clip(jax.random.uniform(streams_of[6], (HEADS,), jnp.float32, -1.0, 1.0) * block_levels(streams_of[6], (HEADS,), ((0, 4),), -0.4, 0.0), -1.0, 1.0)
    head_decay_logarithm = draw_head_decay_logarithm(jax.random.fold_in(streams_of[20], 71), 0)
    value_filter_taps = scatter_about(streams_of[8], (CONV_MIX, INNER), CONV_MIX ** -0.5, 3.0, ((1, 4),))
    write_filter_taps = scatter_about(streams_of[9], (CONV_MIX, GROUPS * STATE), CONV_MIX ** -0.5, 3.0, ((1, 4),))
    read_filter_taps = scatter_about(streams_of[10], (CONV_MIX, GROUPS * STATE), CONV_MIX ** -0.5, 3.0, ((1, 4),))
    gated_group_norm_gain = jnp.clip(1.0 + 0.18 * jax.random.normal(streams_of[11], (INNER,), jnp.float32), 0.1, 1.9)
    mixer_output_weight = scatter_about(streams_of[12], (INNER, D), INNER ** -0.5, 0.125, ((0, 4),))
    residual = scatter_about(streams_of[13], (SEQ, D), 1.0, 6.0, ((0, 8),))
    feedforward_norm_gain = jnp.clip(1.0 + 0.18 * jax.random.normal(streams_of[14], (D,), jnp.float32), 0.1, 1.9)
    feedforward_gate_weight = scatter_about(streams_of[15], (D, FF), D ** -0.5, 0.125, ((0, 8), (1, 4)))
    feedforward_value_weight = scatter_about(streams_of[16], (D, FF), D ** -0.5, 0.125, ((0, 8), (1, 4)))
    gate_filter_taps = scatter_about(streams_of[17], (CONV_FFN, FF), CONV_FFN ** -0.5, 3.5, ((1, 4),))
    single_value_filter_taps = scatter_about(streams_of[18], (CONV_FFN, FF), CONV_FFN ** -0.5, 3.5, ((1, 4),))
    feedforward_down_weight = scatter_about(streams_of[19], (FF, D), FF ** -0.5, 0.078125, ((0, 4), (1, 8)))
    return {"mixer_value_projection": mixer_value_projection, "write_vectors_projected": write_vectors_projected, "read_vectors_projected": read_vectors_projected, "output_gate_projected": output_gate_projected, "step_size_scores": step_size_scores, "position_decay_extra": position_decay_extra, "step_size_bias": step_size_bias, "head_decay_logarithm": head_decay_logarithm, "value_filter_taps": value_filter_taps, "write_filter_taps": write_filter_taps, "read_filter_taps": read_filter_taps, "gated_group_norm_gain": gated_group_norm_gain, "mixer_output_weight": mixer_output_weight, "residual": residual, "feedforward_norm_gain": feedforward_norm_gain, "feedforward_gate_weight": feedforward_gate_weight, "feedforward_value_weight": feedforward_value_weight, "gate_filter_taps": gate_filter_taps, "single_value_filter_taps": single_value_filter_taps, "feedforward_down_weight": feedforward_down_weight}


epsilon = 1e-06

def causal_taps(current, kernel):
    tap_count = kernel.shape[0]
    length = current.shape[0]
    padded = jnp.concatenate([jnp.zeros((tap_count - 1, current.shape[1]), current.dtype), current], 0).astype(jnp.float32)
    result = jnp.zeros((length, current.shape[1]), jnp.float32)
    for offset in range(tap_count):
        result = result + kernel[offset].astype(jnp.float32) * padded[offset:offset + length]
    return result

def channel_norm(stream, gain):
    floats = stream.astype(jnp.float32)
    scaled = floats * lax.rsqrt(lax.optimization_barrier(jnp.mean(floats * floats, axis=-1, keepdims=True)) + epsilon)
    return (scaled * gain).astype(jnp.bfloat16)

def reference(mixer_value_projection, write_vectors_projected, read_vectors_projected, output_gate_projected, step_size_scores, position_decay_extra, step_size_bias, head_decay_logarithm, value_filter_taps, write_filter_taps, read_filter_taps, gated_group_norm_gain, mixer_output_weight, residual, feedforward_norm_gain, feedforward_gate_weight, feedforward_value_weight, gate_filter_taps, single_value_filter_taps, feedforward_down_weight):
    per_group = HEADS // GROUPS
    x_conv = jax.nn.silu(causal_taps(mixer_value_projection, value_filter_taps)).astype(jnp.bfloat16)
    write_conv = jax.nn.silu(causal_taps(write_vectors_projected, write_filter_taps)).astype(jnp.bfloat16)
    read_conv = jax.nn.silu(causal_taps(read_vectors_projected, read_filter_taps)).astype(jnp.bfloat16)
    step_size_head = jax.nn.softplus(step_size_scores + step_size_bias)
    logarithm_decay_rate = -step_size_head * jnp.exp(head_decay_logarithm) + position_decay_extra
    scaled = (x_conv.astype(jnp.float32).reshape(SEQ, HEADS, HEAD) * step_size_head[:, :, None]).astype(jnp.bfloat16)
    block_count = SEQ // BLOCK
    value_blocks = scaled.reshape(block_count, BLOCK, GROUPS, per_group, HEAD)
    write_blocks = write_conv.reshape(block_count, BLOCK, GROUPS, STATE)
    read_blocks = read_conv.reshape(block_count, BLOCK, GROUPS, STATE)
    log_blocks = logarithm_decay_rate.reshape(block_count, BLOCK, HEADS)
    causal = jnp.tril(jnp.ones((BLOCK, BLOCK), dtype=jnp.bool_))

    def block_step(carried, inputs):
        value_rows, write_rows, read_rows, log_rows = inputs
        running = jnp.cumsum(log_rows, axis=0)
        by_head = running.T
        spread = by_head[:, :, None] - by_head[:, None, :]
        decays = jnp.exp(jnp.where(causal, spread, -jnp.inf)).reshape(GROUPS, per_group, BLOCK, BLOCK)
        scores = jnp.einsum('lgn,sgn->gls', read_rows.astype(jnp.float32), write_rows.astype(jnp.float32))
        weights = (scores[:, None] * decays).astype(jnp.bfloat16)
        inside = jnp.einsum('grls,sgrp->lgrp', weights.astype(jnp.float32), value_rows.astype(jnp.float32))
        entering = jnp.einsum('lgn,grnp->lgrp', read_rows.astype(jnp.float32), carried, precision=lax.Precision.HIGHEST)
        entering = entering * jnp.exp(running).reshape(BLOCK, GROUPS, per_group)[..., None]
        tails = jnp.exp(by_head[:, -1:] - by_head).T.reshape(BLOCK, GROUPS, per_group)
        tailed = (value_rows.astype(jnp.float32) * tails[..., None]).astype(jnp.bfloat16)
        fresh = jnp.einsum('sgn,sgrp->grnp', write_rows.astype(jnp.float32), tailed.astype(jnp.float32))
        advanced = carried * jnp.exp(running[-1]).reshape(GROUPS, per_group)[..., None, None] + fresh
        return (advanced, inside + entering)
    start_state = jnp.zeros((GROUPS, per_group, STATE, HEAD), jnp.float32)
    outputs = lax.scan(block_step, start_state, (value_blocks, write_blocks, read_blocks, log_blocks))[1]
    mixer = outputs.reshape(SEQ, INNER)
    gated = (mixer * jax.nn.silu(output_gate_projected.astype(jnp.float32))).reshape(SEQ, GROUPS, INNER // GROUPS)
    gated = gated * lax.rsqrt(lax.optimization_barrier(jnp.mean(gated * gated, axis=-1, keepdims=True)) + epsilon)
    normed = (gated.reshape(SEQ, INNER) * gated_group_norm_gain).astype(jnp.bfloat16)
    stream = (residual.astype(jnp.float32) + jnp.dot(normed, mixer_output_weight, preferred_element_type=jnp.float32)).astype(jnp.bfloat16)
    ffn_in = channel_norm(stream, feedforward_norm_gain)
    gate_rows = jnp.dot(ffn_in, feedforward_gate_weight, preferred_element_type=jnp.float32).astype(jnp.bfloat16)
    value_rows = jnp.dot(ffn_in, feedforward_value_weight, preferred_element_type=jnp.float32).astype(jnp.bfloat16)
    hidden = (jax.nn.silu(causal_taps(gate_rows, gate_filter_taps)) * causal_taps(value_rows, single_value_filter_taps)).astype(jnp.bfloat16)
    down = jnp.dot(hidden, feedforward_down_weight, preferred_element_type=jnp.float32)
    return (stream.astype(jnp.float32) + down).astype(jnp.bfloat16)
```

```python
import jax
import jax.numpy as jnp
from jax import lax
from jax.sharding import PartitionSpec as P

HEAD = 64
STATE = 64
BLOCK = 128


epsilon = 1e-06


def from_behind(value, axis, by):
    length = lax.axis_size(axis)
    pairs = [(i, i + by) for i in range(length) if 0 <= i + by < length]
    return lax.ppermute(value, axis, pairs)


def entering_2(value, axis, join, neutral):
    count, mine = (lax.axis_size(axis), lax.axis_index(axis))

    def shifted(part, by):
        moved = from_behind(part, axis, by)
        return jnp.where(mine >= by, moved, neutral)

    if count == 1:
        return neutral
    window, width = (shifted(value, 1), 1)
    while width < count - 1:
        earlier = shifted(value, 2) if width == 1 else shifted(window, width)
        window, width = (join(earlier, window), 2 * width)
    return window


def halving_bits(axis):
    count = lax.axis_size(axis)
    return [1 << b for b in range(count.bit_length() - 1)] if count & (count - 1) == 0 else None


def swap(value, axis, bit):
    return lax.ppermute(value, axis, [(i, i ^ bit) for i in range(lax.axis_size(axis))])


def product_scattered(rows, weight, axis):
    count, mine = (lax.axis_size(axis), lax.axis_index(axis))
    bits = halving_bits(axis)
    if not bits:
        product = jnp.dot(rows, weight, preferred_element_type=jnp.float32)
        return lax.psum_scatter(product, axis, scatter_dimension=0, tiled=True)
    share = rows.shape[0] // count

    def side(array, which):
        return lax.dynamic_index_in_dim(
            array.reshape(array.shape[0] // 2, 2, *array.shape[1:]),
            which,
            1,
            keepdims=False,
            allow_negative_indices=False,
        )

    rows = rows.reshape(count, share, -1)

    def multiplied(part):
        flat = jnp.dot(
            part.reshape(-1, part.shape[-1]), weight, preferred_element_type=jnp.float32
        )
        return flat.reshape(part.shape[0], share, -1)

    low = mine & 1
    going = multiplied(side(rows, 1 - low)).astype(jnp.bfloat16)
    arrived = swap(going, axis, 1)
    total = multiplied(side(rows, low))
    for bit in bits[1:]:
        own = (mine // bit) & 1
        going = (side(total, 1 - own) + side(arrived, 1 - own).astype(jnp.float32)).astype(
            jnp.bfloat16
        )
        total = side(total, own) + side(arrived, own).astype(jnp.float32)
        arrived = swap(going, axis, bit)
    return (total + arrived.astype(jnp.float32))[0]


def rows_gathered(own, axis):
    bits = halving_bits(axis)
    if not bits:
        return lax.all_gather(own, axis, axis=0, tiled=True)
    mine = lax.axis_index(axis)
    held = own[None]
    for bit in reversed(bits):
        other = swap(held, axis, bit)
        high = ((mine // bit) & 1) == 1
        held = jnp.stack([jnp.where(high, other, held), jnp.where(high, held, other)], 1)
        held = held.reshape(-1, *own.shape)
    return held.reshape(-1, own.shape[-1])


def put(whole, block, index):
    start = (index, *[jnp.zeros_like(index)] * block.ndim)
    return lax.dynamic_update_slice(whole, block[None], start, allow_negative_indices=False)


class RingGather:
    def __init__(self, block, axis):
        self.axis, self.count, self.step = (axis, lax.axis_size(axis), 0)
        count, mine = (self.count, lax.axis_index(axis))
        if count % 2:
            order = list(range(count))
            self.place = mine
        else:
            order = list(range(0, count, 2)) + list(range(count - 1, 0, -2))
            self.place = jnp.where(mine % 2 == 0, mine, 2 * count - 1 - mine) // 2
        self.forward = [(order[p], order[(p + 1) % count]) for p in range(count)]
        self.backward = [(b, a) for a, b in self.forward]
        self.up = self.down = block
        whole = jnp.zeros((count, *block.shape), block.dtype)
        self.whole = put(whole, block, mine)

    def owner(self, place):
        place = lax.rem(place + self.count, self.count)
        if self.count % 2:
            return place
        return jnp.where(2 * place < self.count, 2 * place, 2 * self.count - 1 - 2 * place)

    def advance(self):
        self.step += 1
        if self.step > self.count // 2:
            return
        self.up = lax.ppermute(self.up, self.axis, self.forward)
        self.whole = put(self.whole, self.up, self.owner(self.place - self.step))
        if self.step <= (self.count - 1) // 2:
            self.down = lax.ppermute(self.down, self.axis, self.backward)
            self.whole = put(self.whole, self.down, self.owner(self.place + self.step))

    def settle(self, value):
        value, self.up, self.down = lax.optimization_barrier((value, self.up, self.down))
        return value

    def gathered(self):
        while self.step < self.count // 2:
            self.advance()
        return self.whole.reshape(-1, self.whole.shape[-1])


def causal_taps(current, previous, kernel):
    tap_count = kernel.shape[0]
    length = current.shape[0]
    padded = jnp.concatenate([previous, current], 0).astype(jnp.float32)
    result = jnp.zeros((length, current.shape[1]), jnp.float32)
    for offset in range(tap_count):
        result = result + kernel[offset].astype(jnp.float32) * padded[offset : offset + length]
    return result


def channel_norm(stream, gain):
    floats = stream.astype(jnp.float32)
    scaled = floats * lax.rsqrt(jnp.mean(floats * floats, axis=-1, keepdims=True) + epsilon)
    return (scaled * gain).astype(jnp.bfloat16)


def on_device(
    mixer_value_projection,
    write_vectors_projected,
    read_vectors_projected,
    output_gate_projected,
    step_size_scores,
    position_decay_extra,
    step_size_bias,
    head_decay_logarithm,
    value_filter_taps,
    write_filter_taps,
    read_filter_taps,
    gated_group_norm_gain,
    mixer_output_weight,
    residual,
    feedforward_norm_gain,
    feedforward_gate_weight,
    feedforward_value_weight,
    gate_filter_taps,
    single_value_filter_taps,
    feedforward_down_weight,
):
    row_count = mixer_value_projection.shape[0]
    head_count = step_size_scores.shape[1]
    group_count = write_vectors_projected.shape[1] // STATE
    per_group = head_count // group_count
    mix_rim = value_filter_taps.shape[0] - 1
    channels = (mixer_value_projection.shape[1], write_vectors_projected.shape[1])
    rims = from_behind(
        jnp.concatenate(
            [
                mixer_value_projection[row_count - mix_rim :],
                write_vectors_projected[row_count - mix_rim :],
                read_vectors_projected[row_count - mix_rim :],
            ],
            1,
        ),
        "sp",
        1,
    )
    rim_values, rim_write, rim_read = jnp.split(rims, [channels[0], sum(channels)], axis=1)
    gate_ring = RingGather(feedforward_gate_weight, "sp")
    gate_ring.advance()
    x_conv = jax.nn.silu(causal_taps(mixer_value_projection, rim_values, value_filter_taps)).astype(
        jnp.bfloat16
    )
    write_conv = jax.nn.silu(
        causal_taps(write_vectors_projected, rim_write, write_filter_taps)
    ).astype(jnp.bfloat16)
    read_conv = jax.nn.silu(causal_taps(read_vectors_projected, rim_read, read_filter_taps)).astype(
        jnp.bfloat16
    )
    step_size_head = jax.nn.softplus(step_size_scores + step_size_bias)
    logarithm_decay_rate = -step_size_head * jnp.exp(head_decay_logarithm) + position_decay_extra
    scaled = (
        x_conv.astype(jnp.float32).reshape(row_count, head_count, HEAD) * step_size_head[:, :, None]
    ).astype(jnp.bfloat16)
    block_count = row_count // BLOCK
    value_blocks = scaled.reshape(block_count, BLOCK, group_count, per_group, HEAD)
    write_blocks = write_conv.reshape(block_count, BLOCK, group_count, STATE)
    read_blocks = read_conv.reshape(block_count, BLOCK, group_count, STATE)
    running = jnp.cumsum(logarithm_decay_rate.reshape(block_count, BLOCK, head_count), axis=1)
    by_head = jnp.moveaxis(running, 1, 2)
    spread = by_head[..., :, None] - by_head[..., None, :]
    causal = jnp.tril(jnp.ones((BLOCK, BLOCK), dtype=jnp.bool_))
    decays = jnp.exp(jnp.where(causal, spread, -jnp.inf)).reshape(
        block_count, group_count, per_group, BLOCK, BLOCK
    )
    scores = jnp.einsum(
        "blgn,bsgn->bgls", read_blocks, write_blocks, preferred_element_type=jnp.float32
    )
    weights = (scores[:, :, None] * decays).astype(jnp.bfloat16)
    inside = jnp.einsum(
        "bgrls,bsgrp->blgrp", weights, value_blocks, preferred_element_type=jnp.float32
    )
    tails = jnp.moveaxis(jnp.exp(by_head[..., -1:] - by_head), 2, 1).reshape(
        block_count, BLOCK, group_count, per_group
    )
    tailed = (value_blocks.astype(jnp.float32) * tails[..., None]).astype(jnp.bfloat16)
    fresh = jnp.einsum(
        "bsgn,bsgrp->bgrnp", write_blocks, tailed, preferred_element_type=jnp.float32
    )
    fresh = gate_ring.settle(fresh)
    gate_ring.advance()
    block_logs = by_head[..., -1].reshape(block_count, group_count, per_group)

    empty_state = jnp.zeros((group_count, per_group, STATE, HEAD), jnp.float32)
    block_decays = jnp.exp(block_logs)
    before, carried = ([], empty_state)
    for block in range(block_count):
        before.append(carried)
        carried = carried * block_decays[block][..., None, None] + fresh[block]
    local_before, local_end = (jnp.stack(before), carried)
    device_decay = jnp.exp(jnp.sum(block_logs, axis=0))

    def packed(decay, state):
        row = jnp.broadcast_to(decay[..., None, None], (*decay.shape, 8, HEAD))
        return jnp.concatenate([state, row], 2)

    def combine(earlier, later):
        decay = later[:, :, STATE : STATE + 1]
        state = earlier[:, :, :STATE] * decay + later[:, :, :STATE]
        return jnp.concatenate([state, earlier[:, :, STATE:] * decay], 2)

    identity = packed(jnp.ones((group_count, per_group), jnp.float32), empty_state)
    incoming = entering_2(packed(device_decay, local_end), "sp", combine, identity)[:, :, :STATE]
    incoming = gate_ring.settle(incoming)
    gate_ring.advance()
    before_block = jnp.cumsum(block_logs, axis=0) - block_logs
    entering_state = local_before + incoming[None] * jnp.exp(before_block)[..., None, None]
    entering = jnp.einsum(
        "blgn,bgrnp->blgrp",
        read_blocks.astype(jnp.float32),
        entering_state,
        precision=lax.Precision.HIGHEST,
    )
    entering = (
        entering * jnp.exp(running).reshape(block_count, BLOCK, group_count, per_group)[..., None]
    )
    mixer = (inside + entering).reshape(row_count, head_count * HEAD)
    gated = (mixer * jax.nn.silu(output_gate_projected.astype(jnp.float32))).reshape(
        row_count, group_count, -1
    )
    gated = gated * lax.rsqrt(jnp.mean(gated * gated, axis=-1, keepdims=True) + epsilon)
    normed = (gated.reshape(row_count, -1) * gated_group_norm_gain).astype(jnp.bfloat16)
    share = row_count // lax.axis_size("tp")
    tp_index = lax.axis_index("tp")
    summed = gate_ring.settle(product_scattered(normed, mixer_output_weight, "tp"))
    gate_ring.advance()
    own_residual = lax.dynamic_slice_in_dim(residual, tp_index * share, share, 0)
    stream = (own_residual.astype(jnp.float32) + summed).astype(jnp.bfloat16)
    ffn_rows = rows_gathered(channel_norm(stream, feedforward_norm_gain), "tp")
    gate_full = gate_ring.gathered()
    value_full = lax.all_gather(feedforward_value_weight, "sp", axis=0, tiled=True)
    gate_sum = jnp.dot(ffn_rows, gate_full, preferred_element_type=jnp.float32)
    value_sum = jnp.dot(ffn_rows, value_full, preferred_element_type=jnp.float32)
    gate_rows = gate_sum.astype(jnp.bfloat16)
    value_rows = value_sum.astype(jnp.bfloat16)
    ffn_rim = gate_filter_taps.shape[0] - 1
    rim_gate, rim_value = from_behind(
        (gate_rows[row_count - ffn_rim :], value_rows[row_count - ffn_rim :]), "sp", 1
    )
    hidden = (
        jax.nn.silu(causal_taps(gate_rows, rim_gate, gate_filter_taps))
        * causal_taps(value_rows, rim_value, single_value_filter_taps)
    ).astype(jnp.bfloat16)
    down_full = lax.all_gather(feedforward_down_weight, "sp", axis=1, tiled=True)
    down = product_scattered(hidden, down_full, "tp")
    return (stream.astype(jnp.float32) + down).astype(jnp.bfloat16)


def solution(mesh):
    placed = (
        P("sp", "tp"),
        P("sp", "tp"),
        P("sp", "tp"),
        P("sp", "tp"),
        P("sp", "tp"),
        P("sp", "tp"),
        P("tp"),
        P("tp"),
        P(None, "tp"),
        P(None, "tp"),
        P(None, "tp"),
        P("tp"),
        P("tp", None),
        P("sp", None),
        P(),
        P("sp", "tp"),
        P("sp", "tp"),
        P(None, "tp"),
        P(None, "tp"),
        P("tp", "sp"),
    )
    return jax.shard_map(
        on_device, mesh=mesh, in_specs=placed, out_specs=P(("sp", "tp"), None), check_vma=False
    )
```

```python
import jax
import jax.numpy as jnp
from jax import lax
from jax.sharding import PartitionSpec as P

HEAD = 64
STATE = 64
BLOCK = 128


epsilon = 1e-06


def from_behind(value, axis, by):
    length = lax.axis_size(axis)
    pairs = [(i, i + by) for i in range(length) if 0 <= i + by < length]
    return lax.ppermute(value, axis, pairs)


def entering_2(value, axis, join, neutral):
    count, mine = (lax.axis_size(axis), lax.axis_index(axis))

    def shifted(part, by):
        moved = from_behind(part, axis, by)
        return jnp.where(mine >= by, moved, neutral)

    if count == 1:
        return neutral
    window, width = (shifted(value, 1), 1)
    while width < count - 1:
        earlier = shifted(value, 2) if width == 1 else shifted(window, width)
        window, width = (join(earlier, window), 2 * width)
    return window


def halving_bits(axis):
    count = lax.axis_size(axis)
    return [1 << b for b in range(count.bit_length() - 1)] if count & (count - 1) == 0 else None


def swap(value, axis, bit):
    return lax.ppermute(value, axis, [(i, i ^ bit) for i in range(lax.axis_size(axis))])


def product_scattered(rows, weight, axis):
    count, mine = (lax.axis_size(axis), lax.axis_index(axis))
    bits = halving_bits(axis)
    if not bits:
        product = jnp.dot(rows, weight, preferred_element_type=jnp.float32)
        return lax.psum_scatter(product, axis, scatter_dimension=0, tiled=True)
    share = rows.shape[0] // count

    def side(array, which):
        return lax.dynamic_index_in_dim(
            array.reshape(array.shape[0] // 2, 2, *array.shape[1:]),
            which,
            1,
            keepdims=False,
            allow_negative_indices=False,
        )

    rows = rows.reshape(count, share, -1)

    def multiplied(part):
        flat = jnp.dot(
            part.reshape(-1, part.shape[-1]), weight, preferred_element_type=jnp.float32
        )
        return flat.reshape(part.shape[0], share, -1)

    low = mine & 1
    product = multiplied(rows)
    going = side(product, 1 - low).astype(jnp.bfloat16)
    arrived = swap(going, axis, 1)
    total = side(product, low)
    for bit in bits[1:]:
        own = (mine // bit) & 1
        going = (side(total, 1 - own) + side(arrived, 1 - own).astype(jnp.float32)).astype(
            jnp.bfloat16
        )
        total = side(total, own) + side(arrived, own).astype(jnp.float32)
        arrived = swap(going, axis, bit)
    return (total + arrived.astype(jnp.float32))[0]


def rows_gathered(own, axis):
    bits = halving_bits(axis)
    if not bits:
        return lax.all_gather(own, axis, axis=0, tiled=True)
    mine = lax.axis_index(axis)
    held = own[None]
    for bit in reversed(bits):
        other = swap(held, axis, bit)
        high = ((mine // bit) & 1) == 1
        held = jnp.stack([jnp.where(high, other, held), jnp.where(high, held, other)], 1)
        held = held.reshape(-1, *own.shape)
    return held.reshape(-1, own.shape[-1])


def put(whole, block, index):
    start = (index, *[jnp.zeros_like(index)] * block.ndim)
    return lax.dynamic_update_slice(whole, block[None], start, allow_negative_indices=False)


class RingGather:
    def __init__(self, block, axis):
        self.axis, self.count, self.step = (axis, lax.axis_size(axis), 0)
        count, mine = (self.count, lax.axis_index(axis))
        if count % 2:
            order = list(range(count))
            self.place = mine
        else:
            order = list(range(0, count, 2)) + list(range(count - 1, 0, -2))
            self.place = jnp.where(mine % 2 == 0, mine, 2 * count - 1 - mine) // 2
        self.forward = [(order[p], order[(p + 1) % count]) for p in range(count)]
        self.backward = [(b, a) for a, b in self.forward]
        self.up = self.down = block
        whole = jnp.zeros((count, *block.shape), block.dtype)
        self.whole = put(whole, block, mine)

    def owner(self, place):
        place = lax.rem(place + self.count, self.count)
        if self.count % 2:
            return place
        return jnp.where(2 * place < self.count, 2 * place, 2 * self.count - 1 - 2 * place)

    def advance(self):
        self.step += 1
        if self.step > self.count // 2:
            return
        self.up = lax.ppermute(self.up, self.axis, self.forward)
        self.whole = put(self.whole, self.up, self.owner(self.place - self.step))
        if self.step <= (self.count - 1) // 2:
            self.down = lax.ppermute(self.down, self.axis, self.backward)
            self.whole = put(self.whole, self.down, self.owner(self.place + self.step))

    def settle(self, value):
        value, self.up, self.down = lax.optimization_barrier((value, self.up, self.down))
        return value

    def gathered(self):
        while self.step < self.count // 2:
            self.advance()
        return self.whole.reshape(-1, self.whole.shape[-1])


def causal_taps(current, previous, kernel):
    tap_count = kernel.shape[0]
    length = current.shape[0]
    padded = jnp.concatenate([previous, current], 0).astype(jnp.float32)
    result = jnp.zeros((length, current.shape[1]), jnp.float32)
    for offset in range(tap_count):
        result = result + kernel[offset].astype(jnp.float32) * padded[offset : offset + length]
    return result


def channel_norm(stream, gain):
    floats = stream.astype(jnp.float32)
    scaled = floats * lax.rsqrt(jnp.mean(floats * floats, axis=-1, keepdims=True) + epsilon)
    return (scaled * gain).astype(jnp.bfloat16)


def on_device(
    mixer_value_projection,
    write_vectors_projected,
    read_vectors_projected,
    output_gate_projected,
    step_size_scores,
    position_decay_extra,
    step_size_bias,
    head_decay_logarithm,
    value_filter_taps,
    write_filter_taps,
    read_filter_taps,
    gated_group_norm_gain,
    mixer_output_weight,
    residual,
    feedforward_norm_gain,
    feedforward_gate_weight,
    feedforward_value_weight,
    gate_filter_taps,
    single_value_filter_taps,
    feedforward_down_weight,
):
    row_count = mixer_value_projection.shape[0]
    head_count = step_size_scores.shape[1]
    group_count = write_vectors_projected.shape[1] // STATE
    per_group = head_count // group_count
    mix_rim = value_filter_taps.shape[0] - 1
    channels = (mixer_value_projection.shape[1], write_vectors_projected.shape[1])
    rims = from_behind(
        jnp.concatenate(
            [
                mixer_value_projection[row_count - mix_rim :],
                write_vectors_projected[row_count - mix_rim :],
                read_vectors_projected[row_count - mix_rim :],
            ],
            1,
        ),
        "sp",
        1,
    )
    rim_values, rim_write, rim_read = jnp.split(rims, [channels[0], sum(channels)], axis=1)
    by_ring = feedforward_gate_weight.shape[1] // 256 * 128
    gate_ring = RingGather(feedforward_gate_weight[:, :by_ring], "sp")
    gate_ring.advance()
    x_conv = jax.nn.silu(causal_taps(mixer_value_projection, rim_values, value_filter_taps)).astype(
        jnp.bfloat16
    )
    write_conv = jax.nn.silu(
        causal_taps(write_vectors_projected, rim_write, write_filter_taps)
    ).astype(jnp.bfloat16)
    read_conv = jax.nn.silu(causal_taps(read_vectors_projected, rim_read, read_filter_taps)).astype(
        jnp.bfloat16
    )
    step_size_head = jax.nn.softplus(step_size_scores + step_size_bias)
    logarithm_decay_rate = -step_size_head * jnp.exp(head_decay_logarithm) + position_decay_extra
    scaled = (
        x_conv.astype(jnp.float32).reshape(row_count, head_count, HEAD) * step_size_head[:, :, None]
    ).astype(jnp.bfloat16)
    block_count = row_count // BLOCK
    value_blocks = scaled.reshape(block_count, BLOCK, group_count, per_group, HEAD)
    write_blocks = write_conv.reshape(block_count, BLOCK, group_count, STATE)
    read_blocks = read_conv.reshape(block_count, BLOCK, group_count, STATE)
    running = jnp.cumsum(logarithm_decay_rate.reshape(block_count, BLOCK, head_count), axis=1)
    by_head = jnp.moveaxis(running, 1, 2)
    spread = by_head[..., :, None] - by_head[..., None, :]
    causal = jnp.tril(jnp.ones((BLOCK, BLOCK), dtype=jnp.bool_))
    decays = jnp.exp(jnp.where(causal, spread, -jnp.inf)).reshape(
        block_count, group_count, per_group, BLOCK, BLOCK
    )
    scores = jnp.einsum(
        "blgn,bsgn->bgls", read_blocks, write_blocks, preferred_element_type=jnp.float32
    )
    weights = (scores[:, :, None] * decays).astype(jnp.bfloat16)
    inside = jnp.einsum(
        "bgrls,bsgrp->blgrp", weights, value_blocks, preferred_element_type=jnp.float32
    )
    tails = jnp.moveaxis(jnp.exp(by_head[..., -1:] - by_head), 2, 1).reshape(
        block_count, BLOCK, group_count, per_group
    )
    tailed = (value_blocks.astype(jnp.float32) * tails[..., None]).astype(jnp.bfloat16)
    fresh = jnp.einsum(
        "bsgn,bsgrp->bgrnp", write_blocks, tailed, preferred_element_type=jnp.float32
    )
    fresh = gate_ring.settle(fresh)
    gate_ring.advance()
    block_logs = by_head[..., -1].reshape(block_count, group_count, per_group)

    empty_state = jnp.zeros((group_count, per_group, STATE, HEAD), jnp.float32)
    block_decays = jnp.exp(block_logs)
    before, carried = ([], empty_state)
    for block in range(block_count):
        before.append(carried)
        carried = carried * block_decays[block][..., None, None] + fresh[block]
    local_before, local_end = (jnp.stack(before), carried)
    device_decay = jnp.exp(jnp.sum(block_logs, axis=0))

    def packed(decay, state):
        row = jnp.broadcast_to(decay[..., None, None], (*decay.shape, 8, HEAD))
        return jnp.concatenate([state, row], 2)

    def combine(earlier, later):
        decay = later[:, :, STATE : STATE + 1]
        state = earlier[:, :, :STATE] * decay + later[:, :, :STATE]
        return jnp.concatenate([state, earlier[:, :, STATE:] * decay], 2)

    identity = packed(jnp.ones((group_count, per_group), jnp.float32), empty_state)
    incoming = entering_2(packed(device_decay, local_end), "sp", combine, identity)[:, :, :STATE]
    incoming = gate_ring.settle(incoming)
    gate_ring.advance()
    before_block = jnp.cumsum(block_logs, axis=0) - block_logs
    entering_state = local_before + incoming[None] * jnp.exp(before_block)[..., None, None]
    entering = jnp.einsum(
        "blgn,bgrnp->blgrp",
        read_blocks.astype(jnp.float32),
        entering_state,
        precision=lax.Precision.HIGHEST,
    )
    entering = (
        entering * jnp.exp(running).reshape(block_count, BLOCK, group_count, per_group)[..., None]
    )
    mixer = (inside + entering).reshape(row_count, head_count * HEAD)
    gated = (mixer * jax.nn.silu(output_gate_projected.astype(jnp.float32))).reshape(
        row_count, group_count, -1
    )
    gated = gated * lax.rsqrt(jnp.mean(gated * gated, axis=-1, keepdims=True) + epsilon)
    normed = (gated.reshape(row_count, -1) * gated_group_norm_gain).astype(jnp.bfloat16)
    share = row_count // lax.axis_size("tp")
    tp_index = lax.axis_index("tp")
    normed = gate_ring.settle(normed)
    gate_ring.advance()
    summed = product_scattered(normed, mixer_output_weight, "tp")
    own_residual = lax.dynamic_slice_in_dim(residual, tp_index * share, share, 0)
    stream = (own_residual.astype(jnp.float32) + summed).astype(jnp.bfloat16)
    ffn_rows = rows_gathered(channel_norm(stream, feedforward_norm_gain), "tp")
    gate_rest = lax.all_gather(feedforward_gate_weight[:, by_ring:], "sp", axis=0, tiled=True)
    value_full = lax.all_gather(feedforward_value_weight, "sp", axis=0, tiled=True)
    gate_full = jnp.concatenate([gate_ring.gathered(), gate_rest], 1)
    gate_sum = jnp.dot(ffn_rows, gate_full, preferred_element_type=jnp.float32)
    value_sum = jnp.dot(ffn_rows, value_full, preferred_element_type=jnp.float32)
    gate_rows = gate_sum.astype(jnp.bfloat16)
    value_rows = value_sum.astype(jnp.bfloat16)
    ffn_rim = gate_filter_taps.shape[0] - 1
    rim_gate, rim_value = from_behind(
        (gate_rows[row_count - ffn_rim :], value_rows[row_count - ffn_rim :]), "sp", 1
    )
    hidden = (
        jax.nn.silu(causal_taps(gate_rows, rim_gate, gate_filter_taps))
        * causal_taps(value_rows, rim_value, single_value_filter_taps)
    ).astype(jnp.bfloat16)
    down_full = lax.all_gather(feedforward_down_weight, "sp", axis=1, tiled=True)
    down = product_scattered(hidden, down_full, "tp")
    return (stream.astype(jnp.float32) + down).astype(jnp.bfloat16)


def solution(mesh):
    placed = (
        P("sp", "tp"),
        P("sp", "tp"),
        P("sp", "tp"),
        P("sp", "tp"),
        P("sp", "tp"),
        P("sp", "tp"),
        P("tp"),
        P("tp"),
        P(None, "tp"),
        P(None, "tp"),
        P(None, "tp"),
        P("tp"),
        P("tp", None),
        P("sp", None),
        P(),
        P("sp", "tp"),
        P("sp", "tp"),
        P(None, "tp"),
        P(None, "tp"),
        P("tp", "sp"),
    )
    return jax.shard_map(
        on_device, mesh=mesh, in_specs=placed, out_specs=P(("sp", "tp"), None), check_vma=False
    )
```
